32 devices in a mesh: ep: 4 (over y, x), tp: 8 (over z, core).
Axes of the slice: x: 2, y: 2, z: 4, core: 2. Of those that a mesh axis runs over, the one named last changes fastest.
Arguments:
- tokens: bfloat16 [256, 4096], P(('ep', 'tp')), may hold values from -6 to 6
- rec_state: float32 [256, 2048], P('ep', 'tp'), may hold values from -40 to 40
- conv_state: bfloat16 [256, 3, 2048], P('ep', None, 'tp'), may hold values from -6 to 6
- route_ids: int32 [256, 4], P('ep'), may hold values from 0 to 15, all different within a row; in each aligned block of 8 rows (0 to 7, 8 to 15, ...) at most 2 rows name the same one
- route_weights: float32 [256, 4], P(('ep', 'tp')), may hold values from 0.1 to 1
- first_gain: bfloat16 [4096], replicated, may hold values from 0.099609375 to 1.8984375
- proj_input: bfloat16 [4096, 2048], P(None, 'tp'), may hold values from -0.09375 to 0.09375
- proj_gate: bfloat16 [4096, 2048], P(None, 'tp'), may hold values from -0.09375 to 0.09375
- conv_taps: bfloat16 [4, 2048], replicated, may hold values from -1.5 to 1.5
- decay_logit: float32 [2048], replicated, may hold values from 1 to 6
- block_decay: bfloat16 [16, 128, 128], replicated, may hold values from -0.5 to 0.5
- block_input: bfloat16 [16, 128, 128], replicated, may hold values from -0.5 to 0.5
- rec_gain: bfloat16 [2048], replicated, may hold values from 0.099609375 to 1.8984375
- proj_out: bfloat16 [2048, 4096], P('tp'), may hold values from -0.125 to 0.125
- second_gain: bfloat16 [4096], replicated, may hold values from 0.099609375 to 1.8984375
- expert_gate: bfloat16 [16, 4096, 4096], P('ep', None, 'tp'), may hold values from -0.21875 to 0.21875
- expert_up: bfloat16 [16, 4096, 4096], P('ep', None, 'tp'), may hold values from -0.21875 to 0.21875
- expert_down: bfloat16 [16, 4096, 4096], P('ep', 'tp'), may hold values from -0.0234375 to 0.0234375
Outputs:
- result: bfloat16 [256, 4096], P(('ep', 'tp'))
- new_state: float32 [256, 2048], P('ep', 'tp')
- new_conv: bfloat16 [256, 3, 2048], P('ep', None, 'tp')
The draws below stay inside these ranges and needn't reach their ends.
Inputs may be any that keep to these rules, and one draw needn't show every extreme that they name: `route_ids`: each row names 4 different experts; in the rows of one device (aligned blocks of 8 rows) no expert is named by more than 2 rows, and one is named by exactly 2.
All inputs are finite; a program needn't handle non-finite values.
Results may differ from the reference program's by a relative error of at most 0.025.
Values may be sent and summed in bfloat16 or wider, within the bound.
A program may use at most 128 MiB of HBM per device.

```python
import math
import jax
import jax.numpy as jnp
import numpy as np
from jax import lax

D = 4096
D_REC = 2048
REC_BLOCKS = 16
BLOCK_W = 128
TAPS = 4
FF = 4096
EXPERTS = 16
TOP_K = 4
TOK = 8
CAP = 2
BATCH = 256
N_EP = 4
N_TP = 8


def draw_rec_state(key, part):
    key_base, key_rows = jax.random.split(jax.random.fold_in(key, 11), 2)
    column = jnp.arange(D_REC, dtype=jnp.float32) / D_REC
    column_scale = 0.4 * jnp.exp(column * math.log(8.0))
    row_scale = jnp.exp(jax.random.uniform(key_rows, (BATCH, 1), jnp.float32, math.log(0.3), math.log(3.0)))
    base = jnp.clip(jax.random.normal(key_base, (BATCH, D_REC), jnp.float32), -4.0, 4.0)
    return base * row_scale * column_scale


def steps_of(stream_key, shape, cuts, least, top_value):
    level, own = 1.0, jax.random.fold_in(stream_key, 6)
    for dim, shards_of in cuts:
        draws = jnp.exp(jax.random.uniform(jax.random.fold_in(own, dim), (shards_of,), jnp.float32, least / len(cuts), top_value / len(cuts)))
        level = level * jnp.repeat(draws, shape[dim] // shards_of).reshape([-1 if axis == dim else 1 for axis in range(len(shape))])
    return level


def routed_block(own_key, own, number, rows, number_of, top, most, lean):
    order = jax.random.permutation(own_key, number_of)
    packed, common = shares(number_of, rows * top, most, lean, True), shares(number_of, rows * top, most, lean, False)
    places = jnp.arange(number_of)

    def named(lengths, turn):
        used = int((lengths > 0).sum())
        fixed = max(1, used // 4)
        passed = fixed + (places - fixed + turn * (used - fixed)) % max(1, number_of - fixed)
        return jnp.zeros((number_of,), jnp.int32).at[order[jnp.where(places < fixed, places, passed)]].set(jnp.asarray(lengths, jnp.int32))

    lengths = jnp.where(number % 4 == 0, named(packed, number // 4), named(common, number - number // 4 - 1))
    mixed = jax.random.permutation(jax.random.fold_in(own, 3), number_of)
    donor, receiver = mixed[0:number_of // 2 * 2:2], mixed[1:number_of // 2 * 2:2]
    room = jnp.minimum(lengths[donor] - 1, most - lengths[receiver]) // 2
    room = jnp.where((donor == order[0]) | (receiver == order[0]) | (lengths[receiver] == 0), 0, jnp.maximum(room, 0))
    passed = jax.random.randint(jax.random.fold_in(own, 4), (number_of // 2,), 0, 1 << 20) % (room + 1)
    lengths = lengths.at[donor].add(-passed).at[receiver].add(passed)
    labels = jnp.searchsorted(jnp.cumsum(lengths), jnp.arange(rows * top), side="right").astype(jnp.int32)
    table = labels.reshape(top, rows).T
    table = table[jax.random.permutation(jax.random.fold_in(own, 1), rows)]
    turn = jax.random.randint(jax.random.fold_in(own, 2), (rows, 1), 0, top)
    return jnp.take_along_axis(table, (jnp.arange(top)[None, :] + turn) % top, axis=1)


def shares(count, total, limit, slope, full):
    loads = [(1 << 20) // math.isqrt(grade ** slope) + 1 for grade in range(1, count + 1)]
    largest = limit if full else min(limit, max(-(-total // count), total * loads[0] // sum(loads)))
    least = 1 if total - largest >= count - 1 else 0
    counts, rest = [largest] + [least] * (count - 1), total - largest - least * (count - 1)
    while rest > 0:
        movable = [i for i in range(1, count) if counts[i] < largest] or [i for i in range(1, count) if counts[i] < limit]
        pool, remaining = sum([loads[i] for i in movable]), rest
        for i in movable:
            extra = min(limit - counts[i], max(1, remaining * loads[i] // pool), rest)
            counts[i] = counts[i] + extra
            rest = rest - extra
    return np.array(counts)


def centred(own_key, extent, width, most, cuts=(), held_as=jnp.bfloat16):
    loudness = steps_of(own_key, extent, cuts, -0.22, 0.18) if cuts else 1.0
    entries = jax.random.normal(own_key, extent, jnp.float32) * width * loudness
    return jnp.minimum(jnp.maximum(entries, -most), most).astype(held_as)


def setup_inputs(seed: int = 0) -> dict:
    seeds = jax.random.split(jax.random.key(seed), 19)
    tokens = centred(seeds[0], (BATCH, D), 1.0, 6.0, ((0, 32),))
    rec_state = draw_rec_state(jax.random.fold_in(seeds[18], 71), 0)
    conv_state = centred(seeds[2], (BATCH, TAPS - 1, D_REC), 1.0, 6.0, ((0, 4), (2, 8)))
    route_ids_keys = jax.random.split(jax.random.fold_in(seeds[3], 1), BATCH // TOK)
    route_ids_turns = jax.random.permutation(jax.random.fold_in(seeds[3], 3), BATCH // TOK)
    route_ids = jax.vmap(lambda own, number: routed_block(jax.random.fold_in(seeds[3], 2), own, number, TOK, EXPERTS, TOP_K, CAP, 1))(route_ids_keys, route_ids_turns).reshape((BATCH, TOP_K))
    route_weights = jnp.clip(jnp.exp(math.log(1.0) - 2.3025851 * jax.random.uniform(seeds[4], (BATCH, TOP_K), jnp.float32) ** steps_of(seeds[4], (BATCH, TOP_K), ((0, 32),), -0.2, 0.2)), 0.1, 1.0)
    first_gain = jnp.clip(1.0 + 0.18 * jax.random.normal(seeds[5], (D,), jnp.float32), 0.099609375, 1.8984375).astype(jnp.bfloat16)
    proj_input = centred(seeds[6], (D, D_REC), D ** -0.5, 0.09375, ((1, 8),))
    proj_gate = centred(seeds[7], (D, D_REC), D ** -0.5, 0.09375, ((1, 8),))
    conv_taps = centred(seeds[8], (TAPS, D_REC), 0.25, 1.5)
    decay_logit = jnp.clip(jax.random.uniform(seeds[9], (D_REC,), jnp.float32, 1.0, 6.0), 1.0, 6.0)
    block_decay = centred(seeds[10], (REC_BLOCKS, BLOCK_W, BLOCK_W), BLOCK_W ** -0.5, 0.5)
    block_input = centred(seeds[11], (REC_BLOCKS, BLOCK_W, BLOCK_W), BLOCK_W ** -0.5, 0.5)
    rec_gain = jnp.clip(1.0 + 0.18 * jax.random.normal(seeds[12], (D_REC,), jnp.float32), 0.099609375, 1.8984375).astype(jnp.bfloat16)
    proj_out = centred(seeds[13], (D_REC, D), D_REC ** -0.5, 0.125, ((0, 8),))
    second_gain = jnp.clip(1.0 + 0.18 * jax.random.normal(seeds[14], (D,), jnp.float32), 0.099609375, 1.8984375).astype(jnp.bfloat16)
    expert_gate = centred(seeds[15], (EXPERTS, D, FF), (D // 6) ** -0.5, 0.21875, ((0, 4), (2, 8)))
    expert_up = centred(seeds[16], (EXPERTS, D, FF), (D // 6) ** -0.5, 0.21875, ((0, 4), (2, 8)))
    expert_down = centred(seeds[17], (EXPERTS, FF, D), (FF * 16) ** -0.5, 0.0234375, ((0, 4), (1, 8)))
    return dict(tokens=tokens, rec_state=rec_state, conv_state=conv_state, route_ids=route_ids, route_weights=route_weights, first_gain=first_gain, proj_input=proj_input, proj_gate=proj_gate, conv_taps=conv_taps, decay_logit=decay_logit, block_decay=block_decay, block_input=block_input, rec_gain=rec_gain, proj_out=proj_out, second_gain=second_gain, expert_gate=expert_gate, expert_up=expert_up, expert_down=expert_down)


EPS = 1e-06
CLAMP = 7.0
ALPHA = 1.702
RATE = 8.0

def norm_rows(values, gain):
    scale = lax.rsqrt(lax.optimization_barrier(jnp.mean(values * values, axis=-1, keepdims=True)) + EPS)
    return values * scale * gain.astype(jnp.float32)

def slot_positions(ids, blocks):
    rows, picks = ids.shape
    onehot = (ids[:, :, None] == jnp.arange(EXPERTS, dtype=jnp.int32)).astype(jnp.int32)
    onehot = onehot.reshape(blocks, rows // blocks * picks, EXPERTS)
    before = jnp.cumsum(onehot, axis=1) - onehot
    return lax.optimization_barrier(jnp.sum(before * onehot, axis=-1)).reshape(rows, picks).astype(jnp.int32)

def reference(tokens, rec_state, conv_state, route_ids, route_weights, first_gain, proj_input, proj_gate, conv_taps, decay_logit, block_decay, block_input, rec_gain, proj_out, second_gain, expert_gate, expert_up, expert_down):
    token_values = tokens.astype(jnp.float32)
    normed = norm_rows(token_values, first_gain).astype(jnp.bfloat16)
    branch_in = jnp.dot(normed, proj_input, preferred_element_type=jnp.float32).astype(jnp.bfloat16)
    branch_gate = jnp.dot(normed, proj_gate, preferred_element_type=jnp.float32).astype(jnp.bfloat16)
    tap_weights = conv_taps.astype(jnp.float32)
    conv_values = conv_state.astype(jnp.float32)
    conv_out = tap_weights[TAPS - 1] * branch_in.astype(jnp.float32)
    for tap in range(TAPS - 1):
        conv_out = conv_out + tap_weights[tap] * conv_values[:, tap]
    new_conv = jnp.concatenate([conv_state[:, 1:], branch_in[:, None, :]], axis=1)
    conv_low = lax.optimization_barrier(conv_out.astype(jnp.bfloat16)).astype(jnp.float32)
    blocked = conv_low.reshape(BATCH, REC_BLOCKS, BLOCK_W)
    decay_gate = jax.nn.sigmoid(jnp.einsum('rnk,nkj->rnj', blocked, block_decay.astype(jnp.float32)).reshape(BATCH, D_REC))
    input_gate = jax.nn.sigmoid(jnp.einsum('rnk,nkj->rnj', blocked, block_input.astype(jnp.float32)).reshape(BATCH, D_REC))
    log_keep = -RATE * decay_gate * jax.nn.softplus(-decay_logit)
    keep_factor = jnp.exp(log_keep)
    new_state = keep_factor * rec_state + jnp.sqrt(-jnp.expm1(2.0 * log_keep)) * input_gate * conv_out
    hidden = new_state * jax.nn.gelu(branch_gate.astype(jnp.float32))
    squares = lax.optimization_barrier(jnp.sum(hidden * hidden, axis=-1, keepdims=True))
    gained = (hidden * rec_gain.astype(jnp.float32)).astype(jnp.bfloat16)
    partial_value = jnp.dot(gained, proj_out, preferred_element_type=jnp.float32)
    residual = token_values + partial_value * lax.rsqrt(squares / D_REC + EPS)
    second = norm_rows(residual, second_gain).astype(jnp.bfloat16)
    devices = N_EP * N_TP
    tok_rows = BATCH // devices
    positions = slot_positions(route_ids, devices)
    row_owner = (jnp.arange(BATCH, dtype=jnp.int32) // tok_rows)[:, None]
    slots = row_owner * CAP + positions
    slot_count = devices * CAP
    row_index = jnp.broadcast_to(jnp.arange(BATCH, dtype=jnp.int32)[:, None], route_ids.shape)
    table = jnp.zeros((EXPERTS, slot_count), jnp.int32).at[route_ids, slots].set(row_index)

    def run_expert(expert):
        rows_in = second[table[expert]]
        gate = jnp.dot(rows_in, expert_gate[expert], preferred_element_type=jnp.float32)
        upper = jnp.dot(rows_in, expert_up[expert], preferred_element_type=jnp.float32)
        clipped = jnp.minimum(gate, CLAMP)
        act = ((jnp.clip(upper, -CLAMP, CLAMP) + 1.0) * (clipped * jax.nn.sigmoid(ALPHA * clipped))).astype(jnp.bfloat16)
        pieces = jnp.einsum('rtf,tfd->rtd', act.reshape(slot_count, N_TP, FF // N_TP).astype(jnp.float32), expert_down[expert].reshape(N_TP, FF // N_TP, D).astype(jnp.float32))
        rounded = lax.optimization_barrier(pieces.astype(jnp.bfloat16)).astype(jnp.float32)
        return lax.optimization_barrier(jnp.sum(rounded, axis=1)).astype(jnp.bfloat16)
    outputs = lax.map(run_expert, jnp.arange(EXPERTS, dtype=jnp.int32))
    picked = outputs[route_ids, slots].astype(jnp.float32)
    expert_mix = lax.optimization_barrier(jnp.sum(route_weights[:, :, None] * picked, axis=1))
    result = (residual + expert_mix).astype(jnp.bfloat16)
    return (result, new_state, new_conv)
```

```python
import functools

import jax
import jax.numpy as jnp
from jax import lax
from jax.experimental import pallas as pl
from jax.experimental.pallas import tpu as pltpu
from jax.sharding import PartitionSpec as P

EXPERTS = 16


EPS = 1e-06
CLAMP = 7.0
ALPHA = 1.702
RATE = 8.0


def norm_rows(values, gain):
    scale = lax.rsqrt(jnp.mean(values * values, axis=-1, keepdims=True) + EPS)
    return values * scale * gain.astype(jnp.float32)


def slot_positions(ids, blocks):
    rows, picks = ids.shape
    onehot = (ids[:, :, None] == jnp.arange(EXPERTS, dtype=jnp.int32)).astype(jnp.int32)
    onehot = onehot.reshape(blocks, rows // blocks * picks, EXPERTS)
    before = jnp.cumsum(onehot, axis=1) - onehot
    return jnp.sum(before * onehot, axis=-1).reshape(rows, picks)


def dispatch_rows(slots, rows_in, total):
    hits = (slots[:, :, None] == jnp.arange(total, dtype=jnp.int32)).astype(jnp.bfloat16)
    chooser = jnp.sum(hits, axis=1)
    return jnp.einsum("ns,nd->sd", chooser, rows_in, preferred_element_type=jnp.float32).astype(
        jnp.bfloat16
    )


def run_experts(piece, expert_gate, expert_up, expert_down):
    gate = jnp.einsum("erd,edf->erf", piece, expert_gate, preferred_element_type=jnp.float32)
    upper = jnp.einsum("erd,edf->erf", piece, expert_up, preferred_element_type=jnp.float32)
    clipped = jnp.minimum(gate, CLAMP)
    act = (
        (jnp.clip(upper, -CLAMP, CLAMP) + 1.0) * (clipped * jax.nn.sigmoid(ALPHA * clipped))
    ).astype(jnp.bfloat16)
    return jnp.einsum("erf,efd->erd", act, expert_down, preferred_element_type=jnp.float32)


def collective_plan(
    tokens,
    rec_state,
    conv_state,
    route_ids,
    route_weights,
    first_gain,
    proj_input,
    proj_gate,
    conv_taps,
    decay_logit,
    block_decay,
    block_input,
    rec_gain,
    proj_out,
    second_gain,
    expert_gate,
    expert_up,
    expert_down,
):
    tp_count = lax.axis_size("tp")
    tp_place = lax.axis_index("tp")
    local_width = proj_input.shape[1]
    seq_count = rec_state.shape[0]
    own_count = tokens.shape[0]
    top_count = route_ids.shape[1]
    capacity = max(2, own_count * top_count // EXPERTS)
    first_channel = tp_place * local_width
    own_values = tokens.astype(jnp.float32)
    normed = norm_rows(own_values, first_gain).astype(jnp.bfloat16)
    piece = lax.all_gather(normed, "tp", axis=0, tiled=True)
    both = jnp.concatenate(
        [
            jnp.dot(piece, proj_input, preferred_element_type=jnp.float32),
            jnp.dot(piece, proj_gate, preferred_element_type=jnp.float32),
        ],
        axis=1,
    )
    joined = both.astype(jnp.bfloat16)
    branch_in = joined[:, :local_width]
    branch_gate = joined[:, local_width:]
    tap_weights = lax.dynamic_slice_in_dim(conv_taps, first_channel, local_width, 1).astype(
        jnp.float32
    )
    conv_values = conv_state.astype(jnp.float32)
    conv_output = tap_weights[-1] * branch_in.astype(jnp.float32)
    for tap in range(conv_state.shape[1]):
        conv_output = conv_output + tap_weights[tap] * conv_values[:, tap]
    new_conv = jnp.concatenate([conv_state[:, 1:], branch_in[:, None, :]], axis=1)
    block_width = block_decay.shape[1]
    local_blocks = local_width // block_width
    decay_mats = lax.dynamic_slice_in_dim(block_decay, tp_place * local_blocks, local_blocks, 0)
    input_mats = lax.dynamic_slice_in_dim(block_input, tp_place * local_blocks, local_blocks, 0)
    blocked = conv_output.astype(jnp.bfloat16).reshape(seq_count, local_blocks, block_width)
    decay_gate = jax.nn.sigmoid(
        jnp.einsum("rnk,nkj->rnj", blocked, decay_mats, preferred_element_type=jnp.float32).reshape(
            seq_count, local_width
        )
    )
    input_gate = jax.nn.sigmoid(
        jnp.einsum("rnk,nkj->rnj", blocked, input_mats, preferred_element_type=jnp.float32).reshape(
            seq_count, local_width
        )
    )
    decay_logits = lax.dynamic_slice_in_dim(decay_logit, first_channel, local_width, 0)
    log_keep = -RATE * decay_gate * jax.nn.softplus(-decay_logits)
    keep_factor = jnp.exp(log_keep)
    fresh_input = jnp.sqrt(-jnp.expm1(2.0 * log_keep)) * input_gate * conv_output
    new_state = keep_factor * rec_state + fresh_input
    hidden = new_state * jax.nn.gelu(branch_gate.astype(jnp.float32))
    squares = jnp.sum(hidden * hidden, axis=1, keepdims=True)
    gain_part = lax.dynamic_slice_in_dim(rec_gain, first_channel, local_width, 0).astype(
        jnp.float32
    )
    partial_value = jnp.dot(
        (hidden * gain_part).astype(jnp.bfloat16), proj_out, preferred_element_type=jnp.float32
    )
    channels = local_width * tp_count
    width_out = proj_out.shape[1]
    own_ids = lax.dynamic_slice_in_dim(route_ids, tp_place * own_count, own_count, 0)
    own_slots = own_ids * capacity + slot_positions(own_ids, 1)
    mix_part, own_squares = (
        lax.psum_scatter(
            partial_value.astype(jnp.bfloat16), "tp", scatter_dimension=0, tiled=True
        ).astype(jnp.float32),
        lax.psum_scatter(
            squares.astype(jnp.bfloat16), "tp", scatter_dimension=0, tiled=True
        ).astype(jnp.float32),
    )
    residual = own_values + mix_part * lax.rsqrt(own_squares / channels + EPS)
    second_normed = norm_rows(residual, second_gain).astype(jnp.bfloat16)
    outgoing = dispatch_rows(own_slots, second_normed, EXPERTS * capacity).reshape(
        EXPERTS, capacity, width_out
    )
    arrived = lax.all_to_all(outgoing, "ep", split_axis=0, concat_axis=1, tiled=True)
    partials = run_experts(
        lax.all_gather(arrived, "tp", axis=1, tiled=True), expert_gate, expert_up, expert_down
    )
    summed_rows = lax.psum_scatter(
        partials.astype(jnp.bfloat16), "tp", scatter_dimension=1, tiled=True
    )
    returned = lax.all_to_all(summed_rows, "ep", split_axis=1, concat_axis=0, tiled=True)
    returned_rows = returned.reshape(EXPERTS * capacity, width_out).astype(jnp.float32)
    slot_hits = (own_slots[:, :, None] == jnp.arange(EXPERTS * capacity, dtype=jnp.int32)).astype(
        jnp.float32
    )
    combine_weights = jnp.sum(slot_hits * route_weights[:, :, None], axis=1)
    expert_mix = jnp.dot(combine_weights, returned_rows, precision=lax.Precision.HIGHEST)
    result = (residual + expert_mix).astype(jnp.bfloat16)
    return (result, new_state, new_conv)


MESH = pl.DeviceIdType.MESH
LANES = 128
VMEM_LIMIT = 66_900_000
CHUNKS = 4


def places(z_count):
    ep, tp = lax.axis_index("ep"), lax.axis_index("tp")
    return ep, tp // 2, tp % 2


def remote(src, dst, send_sem, recv_sem, ep, z, core):
    return pltpu.make_async_remote_copy(
        src_ref=src, dst_ref=dst, send_sem=send_sem, recv_sem=recv_sem,
        device_id=(ep, z * 2 + core), device_id_type=MESH,
    )


def rows16(index, count=1):
    return pl.ds(pl.multiple_of(index * 16, 16), 16 * count)


def fold(values):
    half = values.shape[1] // 2
    return jnp.concatenate([values[:, :half], values[:, half:]], axis=0)


def unfold(values):
    half = values.shape[0] // 2
    return jnp.concatenate([values[:half], values[half:]], axis=1)


def split_high_low(values):
    high = values.astype(jnp.bfloat16).astype(jnp.float32)
    return high, values - high


def mix_kernel(
    z_count, channels,
    tokens, gain, conv_base, taps, logit, mats_decay, mats_input, rec_gain, second_gain,
    rec_state, w_in, w_gate, w_out,
    residual_out, second_out, state_out, branch_out,
    xs, v_in, v_gate, v_out, part, from_partner, zsum, from_z,
    w_sem, gz_send, gp_send, g_recv, p_send, p_recv, rz_send, rz_recv,
):
    ep, z, core = places(z_count)
    other = 1 - core
    loads = [
        pltpu.make_async_copy(src, dst, w_sem.at[i])
        for i, (src, dst) in enumerate(((w_in, v_in), (w_gate, v_gate), (w_out, v_out)))
    ]
    for load in loads:
        load.start()
    barrier = pltpu.get_barrier_semaphore()
    pl.semaphore_signal(barrier, inc=1, device_id=(ep, z * 2 + other), device_id_type=MESH)
    for d in range(1, z_count):
        pl.semaphore_signal(
            barrier, inc=1, device_id=(ep, (z + d) % z_count * 2 + core), device_id_type=MESH
        )
    width = tokens.shape[1]
    half = width // 2
    own = tokens[...].astype(jnp.float32)
    me = z * 2 + core
    xs[rows16(me), :] = fold(norm_rows(own, gain[...])).astype(jnp.bfloat16)
    pl.semaphore_wait(barrier, z_count)

    def to_partner(zz):
        block = xs.at[rows16(zz * 2 + core), :]
        return remote(block, block, gp_send.at[zz], g_recv.at[zz * 2 + core], ep, z, other)

    mine = xs.at[rows16(me), :]
    sent = []
    for d in range(1, z_count):
        copy = remote(mine, mine, gz_send.at[d], g_recv.at[me], ep, (z + d) % z_count, core)
        copy.start()
        sent.append(copy)
    copy = to_partner(z)
    copy.start()
    sent.append(copy)
    for d in (1, z_count - 1) + tuple(range(2, z_count - 1)):
        zz = (z + d) % z_count
        block = xs.at[rows16(zz * 2 + core), :]
        remote(block, block, gz_send.at[0], g_recv.at[zz * 2 + core], ep, zz, core).wait_recv()
        copy = to_partner(zz)
        copy.start()
        sent.append(copy)
    for zz in range(z_count):
        block = xs.at[rows16(zz * 2 + other), :]
        remote(block, block, gz_send.at[0], g_recv.at[zz * 2 + other], ep, z, other).wait_recv()
    for copy in sent:
        copy.wait_send()

    blocks = 2 * z_count
    local = w_in.shape[1]
    rows = blocks * 8

    def project(weights):
        top = jnp.dot(xs[...], weights[:half], preferred_element_type=jnp.float32)
        low = jnp.dot(xs[...], weights[half:], preferred_element_type=jnp.float32)
        top = top.reshape(blocks, 16, local)[:, :8]
        low = low.reshape(blocks, 16, local)[:, 8:]
        return (top + low).reshape(rows, local).astype(jnp.bfloat16)

    loads[0].wait()
    branch_in = project(v_in)
    loads[1].wait()
    branch_gate = project(v_gate).astype(jnp.float32)
    branch_out[...] = branch_in
    place = pl.ds(pl.multiple_of(me * local, LANES), local)
    tap = taps[:, place].astype(jnp.float32)
    conv = conv_base[...] + tap[-1:] * branch_in.astype(jnp.float32)
    conv_low = conv.astype(jnp.bfloat16)
    count = local // LANES

    def gates(mats):
        return jax.nn.sigmoid(
            jnp.concatenate(
                [
                    jnp.dot(
                        conv_low[:, i * LANES : (i + 1) * LANES],
                        mats[me * count + i],
                        preferred_element_type=jnp.float32,
                    )
                    for i in range(count)
                ],
                axis=1,
            )
        )

    lam = logit[:, place]
    soft = jnp.log(1.0 + jnp.exp(-jnp.abs(lam))) + jnp.maximum(-lam, 0.0)
    log_keep = -RATE * gates(mats_decay) * soft
    twice = 2.0 * log_keep
    near = -twice * (1.0 + twice * (0.5 + twice * (1.0 / 6.0 + twice * (1.0 / 24.0))))
    rest = jnp.where(twice > -0.03, near, 1.0 - jnp.exp(twice))
    state = jnp.exp(log_keep) * rec_state[...] + jnp.sqrt(rest) * gates(mats_input) * conv
    state_out[...] = state
    hidden = state * jax.nn.gelu(branch_gate)
    squares = jnp.sum(hidden * hidden, axis=1, keepdims=True)
    gained = (hidden * rec_gain[:, place].astype(jnp.float32)).astype(jnp.bfloat16)
    loads[2].wait()

    def store_blocks(columns, top, low):
        for c in range(2):
            for zz in range(z_count):
                b = zz * 2 + c
                piece = jnp.concatenate([top[b * 8 : b * 8 + 8], low[b * 8 : b * 8 + 8]], axis=0)
                first = (c * z_count + zz) * 16
                part[first : first + 16, columns] = piece.astype(jnp.bfloat16)

    step = half // CHUNKS
    for k in range(CHUNKS):
        top = jnp.dot(
            gained, v_out[:, k * step : (k + 1) * step], preferred_element_type=jnp.float32
        )
        low = jnp.dot(
            gained, v_out[:, half + k * step : half + (k + 1) * step],
            preferred_element_type=jnp.float32,
        )
        store_blocks(slice(k * step, (k + 1) * step), top, low)
    high_sq, low_sq = split_high_low(jnp.broadcast_to(squares, (rows, LANES)))
    store_blocks(slice(half, half + LANES), high_sq, low_sq)

    copy = remote(
        part.at[rows16(other * z_count, z_count), :], from_partner, p_send, p_recv, ep, z, other
    )
    copy.start()
    copy.wait()
    zsum[...] = (
        part[rows16(core * z_count, z_count), :].astype(jnp.float32)
        + from_partner[...].astype(jnp.float32)
    ).astype(jnp.bfloat16)
    sent = []
    for d in range(1, z_count):
        zz = (z + d) % z_count
        copy = remote(
            zsum.at[rows16(zz), :], from_z.at[z], rz_send.at[d], rz_recv.at[z], ep, zz, core
        )
        copy.start()
        sent.append(copy)
    total = zsum[rows16(z), :].astype(jnp.float32)
    for d in range(1, z_count):
        zz = (z + d) % z_count
        remote(
            zsum.at[rows16(zz), :], from_z.at[zz], rz_send.at[0], rz_recv.at[zz], ep, zz, core
        ).wait_recv()
        total = total + from_z[zz].astype(jnp.float32)
    for copy in sent:
        copy.wait_send()
    mix = unfold(total[:, :half])
    extra = total[:, half:]
    own_squares = (extra[:8] + extra[8:])[:, :1]
    residual = own + mix * lax.rsqrt(own_squares / channels + EPS)
    residual_out[...] = residual
    second_out[...] = fold(norm_rows(residual, second_gain[...])).astype(jnp.bfloat16)


def expert_kernel(
    z_count, ep_count,
    second, weights, residual, g_hbm, u_hbm, d_hbm,
    result_out,
    xs, vg, vu, vd, chooser, scatter, sel, act, ys, part, from_partner, csum, from_ep, zsum, from_z,
    g_sem, u_sem, d_sem, gz_send, ge_send, gp_send, g_recv,
    p_send, p_recv, re_send, re_recv, rz_send, rz_recv,
):
    ep, z, core = places(z_count)
    other = 1 - core
    experts = g_hbm.shape[0]
    half = second.shape[1]
    shards = 2 * ep_count * z_count

    def load_g(e):
        return pltpu.make_async_copy(g_hbm.at[e], vg.at[e], g_sem.at[e])

    def load_u(e):
        return pltpu.make_async_copy(u_hbm.at[e], vu.at[e], u_sem.at[e])

    def load_d(e):
        return pltpu.make_async_copy(d_hbm.at[e], vd.at[e], d_sem.at[e])

    for e in range(experts):
        load_g(e).start()
        load_u(e).start()
    for e in range(experts):
        load_d(e).start()

    barrier = pltpu.get_barrier_semaphore()
    pl.semaphore_signal(barrier, inc=1, device_id=(ep, z * 2 + other), device_id_type=MESH)
    for d in range(1, z_count):
        pl.semaphore_signal(
            barrier, inc=1, device_id=(ep, (z + d) % z_count * 2 + core), device_id_type=MESH
        )
    for d in range(1, ep_count):
        pl.semaphore_signal(
            barrier, inc=1, device_id=((ep + d) % ep_count, z * 2 + core), device_id_type=MESH
        )

    def shard_of(c, e, zz):
        return (c * ep_count + e) * z_count + zz

    def block_of(c, e, zz):
        return xs.at[rows16(shard_of(c, e, zz)), :]

    me = shard_of(core, ep, z)
    high, low = split_high_low(weights[...])
    xs[rows16(me), :half] = second[...]
    xs[rows16(me), half:] = jnp.concatenate([high, low], axis=0).astype(jnp.bfloat16)
    pl.semaphore_wait(barrier, z_count + ep_count - 1)

    sent = []

    def send(block, send_sem, number, to_ep, to_z, to_core):
        copy = remote(block, block, send_sem, g_recv.at[number], to_ep, to_z, to_core)
        copy.start()
        sent.append(copy)

    def arrived(c, e, zz):
        block = block_of(c, e, zz)
        remote(
            block, block, gz_send.at[0], g_recv.at[shard_of(c, e, zz)], ep, z, other
        ).wait_recv()

    mine = block_of(core, ep, z)
    z_order = (1, z_count - 1) + tuple(range(2, z_count - 1))
    for d in z_order:
        send(mine, gz_send.at[d], me, ep, (z + d) % z_count, core)
    for j in range(1, ep_count):
        send(mine, ge_send.at[0, j], me, (ep + j) % ep_count, z, core)
    send(mine, gp_send.at[0, 0], me, ep, z, other)
    for d in z_order:
        zz = (z + d) % z_count
        arrived(core, ep, zz)
        block, number = block_of(core, ep, zz), shard_of(core, ep, zz)
        for j in range(1, ep_count):
            send(block, ge_send.at[d, j], number, (ep + j) % ep_count, z, core)
        send(block, gp_send.at[d, 0], number, ep, z, other)
    for d in (0,) + z_order:
        zz = (z + d) % z_count
        for j in range(1, ep_count):
            e = (ep + j) % ep_count
            arrived(core, e, zz)
            send(block_of(core, e, zz), gp_send.at[d, j], shard_of(core, e, zz), ep, z, other)
    for e in range(ep_count):
        for zz in range(z_count):
            arrived(other, e, zz)
    for copy in sent:
        copy.wait_send()

    cap = 2
    per_expert = shards * cap
    slots = experts * per_expert
    rows = shards * 16
    extra = xs[:, half:].astype(jnp.float32).reshape(shards, 16, LANES)
    high = jnp.concatenate([extra[:, :8], extra[:, :8]], axis=1).reshape(rows, LANES)
    low = jnp.concatenate([extra[:, 8:], extra[:, 8:]], axis=1).reshape(rows, LANES)
    mask = (high > 0.0).astype(jnp.float32)
    row = lax.broadcasted_iota(jnp.int32, (rows, rows), 0)
    col = lax.broadcasted_iota(jnp.int32, (rows, rows), 1)
    earlier = ((row // 8 == col // 8) & (col < row)).astype(jnp.float32).astype(jnp.bfloat16)
    before = jnp.dot(earlier, mask.astype(jnp.bfloat16), preferred_element_type=jnp.float32)
    name = lax.broadcasted_iota(jnp.int32, (LANES, slots), 0)
    lane = lax.broadcasted_iota(jnp.int32, (LANES, slots), 1)
    spread = (name == ep * experts + lane // per_expert).astype(jnp.float32).astype(jnp.bfloat16)

    def to_slots(values):
        return jnp.dot(values.astype(jnp.bfloat16), spread, preferred_element_type=jnp.float32)

    row = lax.broadcasted_iota(jnp.int32, (rows, slots), 0)
    lane = lax.broadcasted_iota(jnp.int32, (rows, slots), 1)
    wanted = (lane % per_expert - row // 16 * cap).astype(jnp.float32)
    hit = jnp.where(to_slots(mask) > 0.5, 1.0, 0.0) * jnp.where(to_slots(before) == wanted, 1.0, 0.0)
    first = (row % 16 < 8).astype(jnp.float32)
    chooser[0] = (hit * first).T.astype(jnp.bfloat16)
    chooser[1] = (hit * (1.0 - first)).T.astype(jnp.bfloat16)
    share = hit * (to_slots(high) + to_slots(low))
    scatter[...] = (
        share.reshape(shards, 16, slots)[:, :8].reshape(shards * 8, slots).astype(jnp.bfloat16)
    )

    tile = 512

    def choose(i, _):
        at = pl.multiple_of(i * tile, tile)
        values = xs[:, pl.ds(at, tile)]
        for h in range(2):
            sel[:, pl.ds(h * half + at, tile)] = jnp.dot(
                chooser[h], values, preferred_element_type=jnp.float32
            ).astype(jnp.bfloat16)
        return 0

    lax.fori_loop(0, half // tile, choose, 0)

    units = g_hbm.shape[2]
    piece = min(256, units)

    def run(e, _):
        load_g(e).wait()
        load_u(e).wait()
        at = pl.ds(pl.multiple_of(e * per_expert, per_expert), per_expert)
        for n in range(units // piece):
            columns = slice(n * piece, (n + 1) * piece)
            gate = jnp.dot(sel[at, :], vg[e, :, columns], preferred_element_type=jnp.float32)
            upper = jnp.dot(sel[at, :], vu[e, :, columns], preferred_element_type=jnp.float32)
            gate = jnp.minimum(gate, CLAMP)
            act[at, columns] = (
                (jnp.clip(upper, -CLAMP, CLAMP) + 1.0) * (gate * jax.nn.sigmoid(ALPHA * gate))
            ).astype(jnp.bfloat16)
        return 0

    lax.fori_loop(0, experts, run, 0)

    wide = 2 * half // CHUNKS
    narrow = wide // 2
    side = ep_count * z_count
    held = {}

    def produce(k):
        def down(e, _):
            at = pl.ds(pl.multiple_of(e * per_expert, per_expert), per_expert)
            ys[at, :] = jnp.dot(
                act[at, :], vd[e, :, k * wide : (k + 1) * wide],
                preferred_element_type=jnp.float32,
            ).astype(jnp.bfloat16)
            return 0

        if k == 0:
            for e in range(experts):
                load_d(e).wait()
        lax.fori_loop(0, experts, down, 0)
        out = jnp.dot(scatter[...], ys[...], preferred_element_type=jnp.float32)
        out = out.reshape(shards, 8, wide)
        out = jnp.concatenate([out[:, :, :narrow], out[:, :, narrow:]], axis=1)
        part[k] = out.reshape(rows, narrow).astype(jnp.bfloat16)
        copy = remote(
            part.at[k, rows16(other * side, side), :], from_partner.at[k],
            p_send.at[k], p_recv.at[k], ep, z, other,
        )
        copy.start()
        held["p", k] = copy

    def chip_sum(k):
        held["p", k].wait()
        csum[k] = (
            part[k, rows16(core * side, side), :].astype(jnp.float32)
            + from_partner[k].astype(jnp.float32)
        ).astype(jnp.bfloat16)
        for j in range(1, ep_count):
            e = (ep + j) % ep_count
            copy = remote(
                csum.at[k, rows16(e * z_count, z_count), :], from_ep.at[k, ep],
                re_send.at[k, j], re_recv.at[k, ep], e, z, core,
            )
            copy.start()
            held["e", k, j] = copy

    def group_sum(k):
        total = csum[k, rows16(ep * z_count, z_count), :].astype(jnp.float32)
        for j in range(1, ep_count):
            e = (ep + j) % ep_count
            remote(
                csum.at[k, rows16(e * z_count, z_count), :], from_ep.at[k, e],
                re_send.at[k, 0], re_recv.at[k, e], e, z, core,
            ).wait_recv()
            total = total + from_ep[k, e].astype(jnp.float32)
        zsum[k] = total.astype(jnp.bfloat16)
        for d in range(1, z_count):
            zz = (z + d) % z_count
            copy = remote(
                zsum.at[k, rows16(zz), :], from_z.at[k, z],
                rz_send.at[k, d], rz_recv.at[k, z], ep, zz, core,
            )
            copy.start()
            held["z", k, d] = copy

    def finish(k):
        total = zsum[k, rows16(z), :].astype(jnp.float32)
        for d in range(1, z_count):
            zz = (z + d) % z_count
            remote(
                zsum.at[k, rows16(zz), :], from_z.at[k, zz],
                rz_send.at[k, 0], rz_recv.at[k, zz], ep, zz, core,
            ).wait_recv()
            total = total + from_z[k, zz].astype(jnp.float32)
        columns = slice(k * wide, (k + 1) * wide)
        result_out[:, columns] = (residual[:, columns] + unfold(total)).astype(jnp.bfloat16)

    stages = (produce, chip_sum, group_sum, finish)
    for step in range(CHUNKS + len(stages) - 1):
        for lag, stage in enumerate(stages):
            if 0 <= step - lag < CHUNKS:
                stage(step - lag)
    for key, copy in held.items():
        if key[0] != "p":
            copy.wait_send()


def kernel_plan(
    tokens, rec_state, conv_state, route_ids, route_weights, first_gain, proj_input, proj_gate,
    conv_taps, decay_logit, block_decay, block_input, rec_gain, proj_out, second_gain,
    expert_gate, expert_up, expert_down,
):
    tp_count, ep_count = lax.axis_size("tp"), lax.axis_size("ep")
    tp_place = lax.axis_index("tp")
    z_count = tp_count // 2
    own_count, width = tokens.shape
    half = width // 2
    seqs, local = rec_state.shape
    local_experts, _, units = expert_gate.shape
    bf16, f32 = jnp.bfloat16, jnp.float32
    taps = lax.dynamic_slice_in_dim(conv_taps, tp_place * local, local, 1).astype(f32)
    conv_base = jnp.zeros((seqs, local), f32)
    for tap in range(conv_state.shape[1]):
        conv_base = conv_base + taps[tap] * conv_state[:, tap].astype(f32)
    own_ids = lax.dynamic_slice_in_dim(route_ids, tp_place * own_count, own_count, 0)
    named = own_ids[:, :, None] == jnp.arange(LANES, dtype=jnp.int32)
    spread_weights = jnp.sum(jnp.where(named, route_weights[:, :, None], 0.0), axis=1)

    vmem = pl.BlockSpec(memory_space=pltpu.VMEM)
    hbm = pl.BlockSpec(memory_space=pl.ANY)
    dma = pltpu.SemaphoreType.DMA
    group = 16 * tp_count
    residual, second, new_state, branch_in = pl.pallas_call(
        functools.partial(mix_kernel, z_count, local * tp_count),
        out_shape=(
            jax.ShapeDtypeStruct((own_count, width), f32),
            jax.ShapeDtypeStruct((2 * own_count, half), bf16),
            jax.ShapeDtypeStruct((seqs, local), f32),
            jax.ShapeDtypeStruct((seqs, local), bf16),
        ),
        in_specs=[vmem] * 10 + [hbm] * 3,
        out_specs=(vmem,) * 4,
        scratch_shapes=[
            pltpu.VMEM((group, half), bf16),
            pltpu.VMEM((width, local), bf16),
            pltpu.VMEM((width, local), bf16),
            pltpu.VMEM((local, width), bf16),
            pltpu.VMEM((group, half + LANES), bf16),
            pltpu.VMEM((group // 2, half + LANES), bf16),
            pltpu.VMEM((group // 2, half + LANES), bf16),
            pltpu.VMEM((z_count, 16, half + LANES), bf16),
            dma((3,)), dma((z_count,)), dma((z_count,)), dma((tp_count,)),
            dma, dma, dma((z_count,)), dma((z_count,)),
        ],
        compiler_params=pltpu.CompilerParams(
            collective_id=0, has_side_effects=True, vmem_limit_bytes=40_000_000
        ),
        name="mix",
    )(
        tokens, first_gain[None], conv_base, conv_taps, decay_logit[None], block_decay,
        block_input, rec_gain[None], second_gain[None], rec_state, proj_input, proj_gate, proj_out,
    )
    new_conv = jnp.concatenate([conv_state[:, 1:], branch_in[:, None, :]], axis=1)

    shards = tp_count * ep_count
    rows = shards * 16
    side = rows // 2
    slots = local_experts * shards * 2
    wide = width // CHUNKS
    narrow = wide // 2
    result = pl.pallas_call(
        functools.partial(expert_kernel, z_count, ep_count),
        out_shape=jax.ShapeDtypeStruct((own_count, width), bf16),
        in_specs=[vmem] * 3 + [hbm] * 3,
        out_specs=vmem,
        scratch_shapes=[
            pltpu.VMEM((rows, half + LANES), bf16),
            pltpu.VMEM((local_experts, width, units), bf16),
            pltpu.VMEM((local_experts, width, units), bf16),
            pltpu.VMEM((local_experts, units, width), bf16),
            pltpu.VMEM((2, slots, rows), bf16),
            pltpu.VMEM((shards * 8, slots), bf16),
            pltpu.VMEM((slots, width), bf16),
            pltpu.VMEM((slots, units), bf16),
            pltpu.VMEM((slots, wide), bf16),
            pltpu.VMEM((CHUNKS, rows, narrow), bf16),
            pltpu.VMEM((CHUNKS, side, narrow), bf16),
            pltpu.VMEM((CHUNKS, side, narrow), bf16),
            pltpu.VMEM((CHUNKS, ep_count, 16 * z_count, narrow), bf16),
            pltpu.VMEM((CHUNKS, 16 * z_count, narrow), bf16),
            pltpu.VMEM((CHUNKS, z_count, 16, narrow), bf16),
            dma((local_experts,)), dma((local_experts,)), dma((local_experts,)),
            dma((z_count,)), dma((z_count, ep_count)), dma((z_count, ep_count)), dma((shards,)),
            dma((CHUNKS,)), dma((CHUNKS,)),
            dma((CHUNKS, ep_count)), dma((CHUNKS, ep_count)),
            dma((CHUNKS, z_count)), dma((CHUNKS, z_count)),
        ],
        compiler_params=pltpu.CompilerParams(
            collective_id=1, has_side_effects=True, vmem_limit_bytes=VMEM_LIMIT
        ),
        name="experts",
    )(second, spread_weights, residual, expert_gate, expert_up, expert_down)
    return (result, new_state, new_conv)


def per_device(*args):
    tokens, rec_state, ids, block = args[0], args[1], args[3], args[10]
    tp_count, ep_count = lax.axis_size("tp"), lax.axis_size("ep")
    shards = tp_count * ep_count
    expert_rows = args[15].shape[0] * shards * 2
    fits = (
        tokens.shape[0] == 8
        and tp_count % 2 == 0
        and tp_count >= 8
        and max(2, tokens.shape[0] * ids.shape[1] // EXPERTS) == 2
        and expert_rows <= 256
        and block.shape[1] == LANES
        and rec_state.shape[1] % LANES == 0
    )
    return kernel_plan(*args) if fits else collective_plan(*args)


def solution(mesh):
    in_specs = (
        P(("ep", "tp"), None),
        P("ep", "tp"),
        P("ep", None, "tp"),
        P("ep", None),
        P(("ep", "tp"), None),
        P(),
        P(None, "tp"),
        P(None, "tp"),
        P(),
        P(),
        P(),
        P(),
        P(),
        P("tp", None),
        P(),
        P("ep", None, "tp"),
        P("ep", None, "tp"),
        P("ep", "tp", None),
    )
    out_specs = (P(("ep", "tp"), None), P("ep", "tp"), P("ep", None, "tp"))
    return jax.shard_map(
        per_device, mesh=mesh, in_specs=in_specs, out_specs=out_specs, check_vma=False
    )
```

```python
import functools

import jax
import jax.numpy as jnp
from jax import lax
from jax.experimental import pallas as pl
from jax.experimental.pallas import tpu as pltpu
from jax.sharding import PartitionSpec as P

EXPERTS = 16


EPS = 1e-06
CLAMP = 7.0
ALPHA = 1.702
RATE = 8.0


def norm_rows(values, gain):
    scale = lax.rsqrt(jnp.mean(values * values, axis=-1, keepdims=True) + EPS)
    return values * scale * gain.astype(jnp.float32)


def slot_positions(ids, blocks):
    rows, picks = ids.shape
    onehot = (ids[:, :, None] == jnp.arange(EXPERTS, dtype=jnp.int32)).astype(jnp.int32)
    onehot = onehot.reshape(blocks, rows // blocks * picks, EXPERTS)
    before = jnp.cumsum(onehot, axis=1) - onehot
    return jnp.sum(before * onehot, axis=-1).reshape(rows, picks)


def dispatch_rows(slots, rows_in, total):
    hits = (slots[:, :, None] == jnp.arange(total, dtype=jnp.int32)).astype(jnp.bfloat16)
    chooser = jnp.sum(hits, axis=1)
    return jnp.einsum("ns,nd->sd", chooser, rows_in, preferred_element_type=jnp.float32).astype(
        jnp.bfloat16
    )


def run_experts(piece, expert_gate, expert_up, expert_down):
    gate = jnp.einsum("erd,edf->erf", piece, expert_gate, preferred_element_type=jnp.float32)
    upper = jnp.einsum("erd,edf->erf", piece, expert_up, preferred_element_type=jnp.float32)
    clipped = jnp.minimum(gate, CLAMP)
    act = (
        (jnp.clip(upper, -CLAMP, CLAMP) + 1.0) * (clipped * jax.nn.sigmoid(ALPHA * clipped))
    ).astype(jnp.bfloat16)
    return jnp.einsum("erf,efd->erd", act, expert_down, preferred_element_type=jnp.float32)


def collective_plan(
    tokens,
    rec_state,
    conv_state,
    route_ids,
    route_weights,
    first_gain,
    proj_input,
    proj_gate,
    conv_taps,
    decay_logit,
    block_decay,
    block_input,
    rec_gain,
    proj_out,
    second_gain,
    expert_gate,
    expert_up,
    expert_down,
):
    tp_count = lax.axis_size("tp")
    tp_place = lax.axis_index("tp")
    local_width = proj_input.shape[1]
    seq_count = rec_state.shape[0]
    own_count = tokens.shape[0]
    top_count = route_ids.shape[1]
    capacity = max(2, own_count * top_count // EXPERTS)
    first_channel = tp_place * local_width
    own_values = tokens.astype(jnp.float32)
    normed = norm_rows(own_values, first_gain).astype(jnp.bfloat16)
    piece = lax.all_gather(normed, "tp", axis=0, tiled=True)
    both = jnp.concatenate(
        [
            jnp.dot(piece, proj_input, preferred_element_type=jnp.float32),
            jnp.dot(piece, proj_gate, preferred_element_type=jnp.float32),
        ],
        axis=1,
    )
    joined = both.astype(jnp.bfloat16)
    branch_in = joined[:, :local_width]
    branch_gate = joined[:, local_width:]
    tap_weights = lax.dynamic_slice_in_dim(conv_taps, first_channel, local_width, 1).astype(
        jnp.float32
    )
    conv_values = conv_state.astype(jnp.float32)
    conv_output = tap_weights[-1] * branch_in.astype(jnp.float32)
    for tap in range(conv_state.shape[1]):
        conv_output = conv_output + tap_weights[tap] * conv_values[:, tap]
    new_conv = jnp.concatenate([conv_state[:, 1:], branch_in[:, None, :]], axis=1)
    block_width = block_decay.shape[1]
    local_blocks = local_width // block_width
    decay_mats = lax.dynamic_slice_in_dim(block_decay, tp_place * local_blocks, local_blocks, 0)
    input_mats = lax.dynamic_slice_in_dim(block_input, tp_place * local_blocks, local_blocks, 0)
    blocked = conv_output.astype(jnp.bfloat16).reshape(seq_count, local_blocks, block_width)
    decay_gate = jax.nn.sigmoid(
        jnp.einsum("rnk,nkj->rnj", blocked, decay_mats, preferred_element_type=jnp.float32).reshape(
            seq_count, local_width
        )
    )
    input_gate = jax.nn.sigmoid(
        jnp.einsum("rnk,nkj->rnj", blocked, input_mats, preferred_element_type=jnp.float32).reshape(
            seq_count, local_width
        )
    )
    decay_logits = lax.dynamic_slice_in_dim(decay_logit, first_channel, local_width, 0)
    log_keep = -RATE * decay_gate * jax.nn.softplus(-decay_logits)
    keep_factor = jnp.exp(log_keep)
    fresh_input = jnp.sqrt(-jnp.expm1(2.0 * log_keep)) * input_gate * conv_output
    new_state = keep_factor * rec_state + fresh_input
    hidden = new_state * jax.nn.gelu(branch_gate.astype(jnp.float32))
    squares = jnp.sum(hidden * hidden, axis=1, keepdims=True)
    gain_part = lax.dynamic_slice_in_dim(rec_gain, first_channel, local_width, 0).astype(
        jnp.float32
    )
    partial_value = jnp.dot(
        (hidden * gain_part).astype(jnp.bfloat16), proj_out, preferred_element_type=jnp.float32
    )
    channels = local_width * tp_count
    width_out = proj_out.shape[1]
    own_ids = lax.dynamic_slice_in_dim(route_ids, tp_place * own_count, own_count, 0)
    own_slots = own_ids * capacity + slot_positions(own_ids, 1)
    mix_part, own_squares = (
        lax.psum_scatter(
            partial_value.astype(jnp.bfloat16), "tp", scatter_dimension=0, tiled=True
        ).astype(jnp.float32),
        lax.psum_scatter(
            squares.astype(jnp.bfloat16), "tp", scatter_dimension=0, tiled=True
        ).astype(jnp.float32),
    )
    residual = own_values + mix_part * lax.rsqrt(own_squares / channels + EPS)
    second_normed = norm_rows(residual, second_gain).astype(jnp.bfloat16)
    outgoing = dispatch_rows(own_slots, second_normed, EXPERTS * capacity).reshape(
        EXPERTS, capacity, width_out
    )
    arrived = lax.all_to_all(outgoing, "ep", split_axis=0, concat_axis=1, tiled=True)
    partials = run_experts(
        lax.all_gather(arrived, "tp", axis=1, tiled=True), expert_gate, expert_up, expert_down
    )
    summed_rows = lax.psum_scatter(
        partials.astype(jnp.bfloat16), "tp", scatter_dimension=1, tiled=True
    )
    returned = lax.all_to_all(summed_rows, "ep", split_axis=1, concat_axis=0, tiled=True)
    returned_rows = returned.reshape(EXPERTS * capacity, width_out).astype(jnp.float32)
    slot_hits = (own_slots[:, :, None] == jnp.arange(EXPERTS * capacity, dtype=jnp.int32)).astype(
        jnp.float32
    )
    combine_weights = jnp.sum(slot_hits * route_weights[:, :, None], axis=1)
    expert_mix = jnp.dot(combine_weights, returned_rows, precision=lax.Precision.HIGHEST)
    result = (residual + expert_mix).astype(jnp.bfloat16)
    return (result, new_state, new_conv)


MESH = pl.DeviceIdType.MESH
LANES = 128
VMEM_LIMIT = 66_900_000
CHUNKS = 4


def places(z_count):
    ep, tp = lax.axis_index("ep"), lax.axis_index("tp")
    return ep, tp // 2, tp % 2


def remote(src, dst, send_sem, recv_sem, ep, z, core):
    return pltpu.make_async_remote_copy(
        src_ref=src, dst_ref=dst, send_sem=send_sem, recv_sem=recv_sem,
        device_id=(ep, z * 2 + core), device_id_type=MESH,
    )


def rows16(index, count=1):
    return pl.ds(pl.multiple_of(index * 16, 16), 16 * count)


def fold(values):
    half = values.shape[1] // 2
    return jnp.concatenate([values[:, :half], values[:, half:]], axis=0)


def unfold(values):
    half = values.shape[0] // 2
    return jnp.concatenate([values[:half], values[half:]], axis=1)


def split_high_low(values):
    high = values.astype(jnp.bfloat16).astype(jnp.float32)
    return high, values - high


def mix_kernel(
    z_count, channels,
    gain, logit, rec_gain, second_gain,
    tokens_hbm, conv_hbm, taps_hbm, decay_hbm, input_hbm, state_hbm, w_in, w_gate, w_out,
    residual_out, second_out, state_out, conv_out,
    tokens, old_conv, taps, mats_decay, mats_input, rec_state, small_sem, xs, v_in, v_gate, v_out, part, from_partner, zsum, from_z,
    w_sem, gz_send, gp_send, g_recv, p_send, p_recv, rz_send, rz_recv,
):
    ep, z, core = places(z_count)
    other = 1 - core
    me = z * 2 + core
    count = mats_decay.shape[0]
    at_blocks = pl.ds(me * count, count)
    small = [
        pltpu.make_async_copy(src, dst, small_sem.at[i])
        for i, (src, dst) in enumerate(
            (
                (tokens_hbm, tokens), (conv_hbm, old_conv), (taps_hbm, taps),
                (decay_hbm.at[at_blocks], mats_decay), (input_hbm.at[at_blocks], mats_input),
                (state_hbm, rec_state),
            )
        )
    ]
    for load in small:
        load.start()
    loads = [
        pltpu.make_async_copy(src, dst, w_sem.at[i])
        for i, (src, dst) in enumerate(((w_in, v_in), (w_gate, v_gate), (w_out, v_out)))
    ]
    for load in loads:
        load.start()
    barrier = pltpu.get_barrier_semaphore()
    pl.semaphore_signal(barrier, inc=1, device_id=(ep, z * 2 + other), device_id_type=MESH)
    for d in range(1, z_count):
        pl.semaphore_signal(
            barrier, inc=1, device_id=(ep, (z + d) % z_count * 2 + core), device_id_type=MESH
        )
    width = tokens.shape[1]
    half = width // 2
    small[0].wait()
    own = tokens[...].astype(jnp.float32)
    xs[rows16(me), :] = fold(norm_rows(own, gain[...].astype(jnp.float32).reshape(1, width))).astype(jnp.bfloat16)
    pl.semaphore_wait(barrier, z_count)

    def to_partner(zz):
        block = xs.at[rows16(zz * 2 + core), :]
        return remote(block, block, gp_send.at[zz], g_recv.at[zz * 2 + core], ep, z, other)

    mine = xs.at[rows16(me), :]
    sent = []
    for d in range(1, z_count):
        copy = remote(mine, mine, gz_send.at[d], g_recv.at[me], ep, (z + d) % z_count, core)
        copy.start()
        sent.append(copy)
    copy = to_partner(z)
    copy.start()
    sent.append(copy)
    for d in (1, z_count - 1) + tuple(range(2, z_count - 1)):
        zz = (z + d) % z_count
        block = xs.at[rows16(zz * 2 + core), :]
        remote(block, block, gz_send.at[0], g_recv.at[zz * 2 + core], ep, zz, core).wait_recv()
        copy = to_partner(zz)
        copy.start()
        sent.append(copy)
    for zz in range(z_count):
        block = xs.at[rows16(zz * 2 + other), :]
        remote(block, block, gz_send.at[0], g_recv.at[zz * 2 + other], ep, z, other).wait_recv()
    for copy in sent:
        copy.wait_send()

    blocks = 2 * z_count
    local = w_in.shape[1]
    rows = blocks * 8

    def project(weights):
        top = jnp.dot(xs[...], weights[:half], preferred_element_type=jnp.float32)
        low = jnp.dot(xs[...], weights[half:], preferred_element_type=jnp.float32)
        top = top.reshape(blocks, 16, local)[:, :8]
        low = low.reshape(blocks, 16, local)[:, 8:]
        return (top + low).reshape(rows, local).astype(jnp.bfloat16)

    loads[0].wait()
    branch_in = project(v_in)
    loads[1].wait()
    branch_gate = project(v_gate).astype(jnp.float32)
    for load in small[1:]:
        load.wait()
    kept = old_conv.shape[0]
    for i in range(kept - 1):
        conv_out[i] = old_conv[i + 1]
    conv_out[kept - 1] = branch_in
    place = pl.ds(pl.multiple_of(me * local, LANES), local)
    tap = taps[:, place].astype(jnp.float32)
    conv = tap[-1:] * branch_in.astype(jnp.float32)
    for i in range(kept):
        conv = conv + tap[i : i + 1] * old_conv[i].astype(jnp.float32)
    conv_low = conv.astype(jnp.bfloat16)

    def gates(mats):
        return jax.nn.sigmoid(
            jnp.concatenate(
                [
                    jnp.dot(
                        conv_low[:, i * LANES : (i + 1) * LANES],
                        mats[i],
                        preferred_element_type=jnp.float32,
                    )
                    for i in range(count)
                ],
                axis=1,
            )
        )

    lam = logit[:, place]
    soft = jnp.log(1.0 + jnp.exp(-jnp.abs(lam))) + jnp.maximum(-lam, 0.0)
    log_keep = -RATE * gates(mats_decay) * soft
    twice = 2.0 * log_keep
    near = -twice * (1.0 + twice * (0.5 + twice * (1.0 / 6.0 + twice * (1.0 / 24.0))))
    rest = jnp.where(twice > -0.03, near, 1.0 - jnp.exp(twice))
    state = jnp.exp(log_keep) * rec_state[...] + jnp.sqrt(rest) * gates(mats_input) * conv
    state_out[...] = state
    hidden = state * jax.nn.gelu(branch_gate)
    squares = jnp.sum(hidden * hidden, axis=1, keepdims=True)
    gained = (hidden * rec_gain[:, place].astype(jnp.float32)).astype(jnp.bfloat16)
    loads[2].wait()

    def store_blocks(columns, top, low):
        for c in range(2):
            for zz in range(z_count):
                b = zz * 2 + c
                piece = jnp.concatenate([top[b * 8 : b * 8 + 8], low[b * 8 : b * 8 + 8]], axis=0)
                first = (c * z_count + zz) * 16
                part[first : first + 16, columns] = piece.astype(jnp.bfloat16)

    step = half // CHUNKS
    for k in range(CHUNKS):
        top = jnp.dot(
            gained, v_out[:, k * step : (k + 1) * step], preferred_element_type=jnp.float32
        )
        low = jnp.dot(
            gained, v_out[:, half + k * step : half + (k + 1) * step],
            preferred_element_type=jnp.float32,
        )
        store_blocks(slice(k * step, (k + 1) * step), top, low)
    high_sq, low_sq = split_high_low(jnp.broadcast_to(squares, (rows, LANES)))
    store_blocks(slice(half, half + LANES), high_sq, low_sq)

    copy = remote(
        part.at[rows16(other * z_count, z_count), :], from_partner, p_send, p_recv, ep, z, other
    )
    copy.start()
    copy.wait()
    zsum[...] = (
        part[rows16(core * z_count, z_count), :].astype(jnp.float32)
        + from_partner[...].astype(jnp.float32)
    ).astype(jnp.bfloat16)
    sent = []
    for d in range(1, z_count):
        zz = (z + d) % z_count
        copy = remote(
            zsum.at[rows16(zz), :], from_z.at[z], rz_send.at[d], rz_recv.at[z], ep, zz, core
        )
        copy.start()
        sent.append(copy)
    total = zsum[rows16(z), :].astype(jnp.float32)
    for d in range(1, z_count):
        zz = (z + d) % z_count
        remote(
            zsum.at[rows16(zz), :], from_z.at[zz], rz_send.at[0], rz_recv.at[zz], ep, zz, core
        ).wait_recv()
        total = total + from_z[zz].astype(jnp.float32)
    for copy in sent:
        copy.wait_send()
    mix = unfold(total[:, :half])
    extra = total[:, half:]
    own_squares = (extra[:8] + extra[8:])[:, :1]
    residual = own + mix * lax.rsqrt(own_squares / channels + EPS)
    residual_out[...] = residual
    second_out[...] = fold(norm_rows(residual, second_gain[...].astype(jnp.float32).reshape(1, width))).astype(jnp.bfloat16)


def expert_kernel(
    z_count, ep_count,
    weights, second, residual_hbm, g_hbm, u_hbm, d_hbm,
    result_out,
    residual, small_sem, xs, vg, vu, vd, chooser, scatter, sel, act, ys, part, from_partner, csum, from_ep, zsum, from_z,
    g_sem, u_sem, d_sem, gz_send, ge_send, gp_send, g_recv,
    p_send, p_recv, re_send, re_recv, rz_send, rz_recv,
):
    ep, z, core = places(z_count)
    other = 1 - core
    experts = g_hbm.shape[0]
    half = second.shape[1]
    shards = 2 * ep_count * z_count

    own_place = (core * ep_count + ep) * z_count + z
    own_rows = pltpu.make_async_copy(
        second, xs.at[rows16(own_place), pl.ds(0, half)], small_sem.at[0]
    )
    own_rows.start()
    own_residual = pltpu.make_async_copy(residual_hbm, residual, small_sem.at[1])

    def load_g(e):
        return pltpu.make_async_copy(g_hbm.at[e], vg.at[e], g_sem.at[e])

    def load_u(e):
        return pltpu.make_async_copy(u_hbm.at[e], vu.at[e], u_sem.at[e])

    def load_d(e):
        return pltpu.make_async_copy(d_hbm.at[e], vd.at[e], d_sem.at[e])

    for e in range(experts):
        load_g(e).start()
        load_u(e).start()
    for e in range(experts):
        load_d(e).start()

    barrier = pltpu.get_barrier_semaphore()
    pl.semaphore_signal(barrier, inc=1, device_id=(ep, z * 2 + other), device_id_type=MESH)
    for d in range(1, z_count):
        pl.semaphore_signal(
            barrier, inc=1, device_id=(ep, (z + d) % z_count * 2 + core), device_id_type=MESH
        )
    for d in range(1, ep_count):
        pl.semaphore_signal(
            barrier, inc=1, device_id=((ep + d) % ep_count, z * 2 + core), device_id_type=MESH
        )

    def shard_of(c, e, zz):
        return (c * ep_count + e) * z_count + zz

    def block_of(c, e, zz):
        return xs.at[rows16(shard_of(c, e, zz)), :]

    me = shard_of(core, ep, z)
    high, low = split_high_low(weights[...])
    xs[rows16(me), half:] = jnp.concatenate([high, low], axis=0).astype(jnp.bfloat16)
    own_rows.wait()
    own_residual.start()
    pl.semaphore_wait(barrier, z_count + ep_count - 1)

    sent = []

    def send(block, send_sem, number, to_ep, to_z, to_core):
        copy = remote(block, block, send_sem, g_recv.at[number], to_ep, to_z, to_core)
        copy.start()
        sent.append(copy)

    def arrived(c, e, zz):
        block = block_of(c, e, zz)
        remote(
            block, block, gz_send.at[0], g_recv.at[shard_of(c, e, zz)], ep, z, other
        ).wait_recv()

    mine = block_of(core, ep, z)
    z_order = (1, z_count - 1) + tuple(range(2, z_count - 1))
    for d in z_order:
        send(mine, gz_send.at[d], me, ep, (z + d) % z_count, core)
    for j in range(1, ep_count):
        send(mine, ge_send.at[0, j], me, (ep + j) % ep_count, z, core)
    send(mine, gp_send.at[0, 0], me, ep, z, other)
    for d in z_order:
        zz = (z + d) % z_count
        arrived(core, ep, zz)
        block, number = block_of(core, ep, zz), shard_of(core, ep, zz)
        for j in range(1, ep_count):
            send(block, ge_send.at[d, j], number, (ep + j) % ep_count, z, core)
        send(block, gp_send.at[d, 0], number, ep, z, other)
    for d in (0,) + z_order:
        zz = (z + d) % z_count
        for j in range(1, ep_count):
            e = (ep + j) % ep_count
            arrived(core, e, zz)
            send(block_of(core, e, zz), gp_send.at[d, j], shard_of(core, e, zz), ep, z, other)
    for e in range(ep_count):
        for zz in range(z_count):
            arrived(other, e, zz)
    for copy in sent:
        copy.wait_send()

    cap = 2
    per_expert = shards * cap
    slots = experts * per_expert
    rows = shards * 16
    extra = xs[:, half:].astype(jnp.float32).reshape(shards, 16, LANES)
    high = jnp.concatenate([extra[:, :8], extra[:, :8]], axis=1).reshape(rows, LANES)
    low = jnp.concatenate([extra[:, 8:], extra[:, 8:]], axis=1).reshape(rows, LANES)
    mask = (high > 0.0).astype(jnp.float32)
    row = lax.broadcasted_iota(jnp.int32, (rows, rows), 0)
    col = lax.broadcasted_iota(jnp.int32, (rows, rows), 1)
    earlier = ((row // 8 == col // 8) & (col < row)).astype(jnp.float32).astype(jnp.bfloat16)
    before = jnp.dot(earlier, mask.astype(jnp.bfloat16), preferred_element_type=jnp.float32)
    name = lax.broadcasted_iota(jnp.int32, (LANES, slots), 0)
    lane = lax.broadcasted_iota(jnp.int32, (LANES, slots), 1)
    spread = (name == ep * experts + lane // per_expert).astype(jnp.float32).astype(jnp.bfloat16)

    def to_slots(values):
        return jnp.dot(values.astype(jnp.bfloat16), spread, preferred_element_type=jnp.float32)

    row = lax.broadcasted_iota(jnp.int32, (rows, slots), 0)
    lane = lax.broadcasted_iota(jnp.int32, (rows, slots), 1)
    wanted = (lane % per_expert - row // 16 * cap).astype(jnp.float32)
    hit = jnp.where(to_slots(mask) > 0.5, 1.0, 0.0) * jnp.where(to_slots(before) == wanted, 1.0, 0.0)
    first = (row % 16 < 8).astype(jnp.float32)
    chooser[0] = (hit * first).T.astype(jnp.bfloat16)
    chooser[1] = (hit * (1.0 - first)).T.astype(jnp.bfloat16)
    share = hit * (to_slots(high) + to_slots(low))
    scatter[...] = (
        share.reshape(shards, 16, slots)[:, :8].reshape(shards * 8, slots).astype(jnp.bfloat16)
    )

    tile = 512

    def choose(i, _):
        at = pl.multiple_of(i * tile, tile)
        values = xs[:, pl.ds(at, tile)]
        for h in range(2):
            sel[:, pl.ds(h * half + at, tile)] = jnp.dot(
                chooser[h], values, preferred_element_type=jnp.float32
            ).astype(jnp.bfloat16)
        return 0

    lax.fori_loop(0, half // tile, choose, 0)

    units = g_hbm.shape[2]
    piece = min(256, units)

    def run(e, _):
        load_g(e).wait()
        load_u(e).wait()
        at = pl.ds(pl.multiple_of(e * per_expert, per_expert), per_expert)
        for n in range(units // piece):
            columns = slice(n * piece, (n + 1) * piece)
            gate = jnp.dot(sel[at, :], vg[e, :, columns], preferred_element_type=jnp.float32)
            upper = jnp.dot(sel[at, :], vu[e, :, columns], preferred_element_type=jnp.float32)
            gate = jnp.minimum(gate, CLAMP)
            act[at, columns] = (
                (jnp.clip(upper, -CLAMP, CLAMP) + 1.0) * (gate * jax.nn.sigmoid(ALPHA * gate))
            ).astype(jnp.bfloat16)
        return 0

    lax.fori_loop(0, experts, run, 0)

    wide = 2 * half // CHUNKS
    narrow = wide // 2
    side = ep_count * z_count
    held = {}

    def produce(k):
        def down(e, _):
            at = pl.ds(pl.multiple_of(e * per_expert, per_expert), per_expert)
            ys[at, :] = jnp.dot(
                act[at, :], vd[e, :, k * wide : (k + 1) * wide],
                preferred_element_type=jnp.float32,
            ).astype(jnp.bfloat16)
            return 0

        if k == 0:
            for e in range(experts):
                load_d(e).wait()
        lax.fori_loop(0, experts, down, 0)
        out = jnp.dot(scatter[...], ys[...], preferred_element_type=jnp.float32)
        out = out.reshape(shards, 8, wide)
        out = jnp.concatenate([out[:, :, :narrow], out[:, :, narrow:]], axis=1)
        part[k] = out.reshape(rows, narrow).astype(jnp.bfloat16)
        copy = remote(
            part.at[k, rows16(other * side, side), :], from_partner.at[k],
            p_send.at[k], p_recv.at[k], ep, z, other,
        )
        copy.start()
        held["p", k] = copy

    def chip_sum(k):
        held["p", k].wait()
        csum[k] = (
            part[k, rows16(core * side, side), :].astype(jnp.float32)
            + from_partner[k].astype(jnp.float32)
        ).astype(jnp.bfloat16)
        for j in range(1, ep_count):
            e = (ep + j) % ep_count
            copy = remote(
                csum.at[k, rows16(e * z_count, z_count), :], from_ep.at[k, ep],
                re_send.at[k, j], re_recv.at[k, ep], e, z, core,
            )
            copy.start()
            held["e", k, j] = copy

    def group_sum(k):
        total = csum[k, rows16(ep * z_count, z_count), :].astype(jnp.float32)
        for j in range(1, ep_count):
            e = (ep + j) % ep_count
            remote(
                csum.at[k, rows16(e * z_count, z_count), :], from_ep.at[k, e],
                re_send.at[k, 0], re_recv.at[k, e], e, z, core,
            ).wait_recv()
            total = total + from_ep[k, e].astype(jnp.float32)
        zsum[k] = total.astype(jnp.bfloat16)
        for d in range(1, z_count):
            zz = (z + d) % z_count
            copy = remote(
                zsum.at[k, rows16(zz), :], from_z.at[k, z],
                rz_send.at[k, d], rz_recv.at[k, z], ep, zz, core,
            )
            copy.start()
            held["z", k, d] = copy

    def finish(k):
        if k == 0:
            own_residual.wait()
        total = zsum[k, rows16(z), :].astype(jnp.float32)
        for d in range(1, z_count):
            zz = (z + d) % z_count
            remote(
                zsum.at[k, rows16(zz), :], from_z.at[k, zz],
                rz_send.at[k, 0], rz_recv.at[k, zz], ep, zz, core,
            ).wait_recv()
            total = total + from_z[k, zz].astype(jnp.float32)
        columns = slice(k * wide, (k + 1) * wide)
        result_out[:, columns] = (residual[:, columns] + unfold(total)).astype(jnp.bfloat16)

    stages = (produce, chip_sum, group_sum, finish)
    for step in range(CHUNKS + len(stages) - 1):
        for lag, stage in enumerate(stages):
            if 0 <= step - lag < CHUNKS:
                stage(step - lag)
    for key, copy in held.items():
        if key[0] != "p":
            copy.wait_send()


def kernel_plan(
    tokens, rec_state, conv_state, route_ids, route_weights, first_gain, proj_input, proj_gate,
    conv_taps, decay_logit, block_decay, block_input, rec_gain, proj_out, second_gain,
    expert_gate, expert_up, expert_down,
):
    tp_count, ep_count = lax.axis_size("tp"), lax.axis_size("ep")
    tp_place = lax.axis_index("tp")
    z_count = tp_count // 2
    own_count, width = tokens.shape
    half = width // 2
    seqs, local = rec_state.shape
    local_experts, _, units = expert_gate.shape
    bf16, f32 = jnp.bfloat16, jnp.float32
    kept = conv_state.shape[1]
    own_ids = lax.dynamic_slice_in_dim(route_ids, tp_place * own_count, own_count, 0)
    named = own_ids[:, :, None] == jnp.arange(LANES, dtype=jnp.int32)
    spread_weights = jnp.sum(jnp.where(named, route_weights[:, :, None], 0.0), axis=1)

    vmem = pl.BlockSpec(memory_space=pltpu.VMEM)
    hbm = pl.BlockSpec(memory_space=pl.ANY)
    dma = pltpu.SemaphoreType.DMA
    group = 16 * tp_count
    residual, second, new_state, conv_major = pl.pallas_call(
        functools.partial(mix_kernel, z_count, local * tp_count),
        out_shape=(
            jax.ShapeDtypeStruct((own_count, width), f32),
            jax.ShapeDtypeStruct((2 * own_count, half), bf16),
            jax.ShapeDtypeStruct((seqs, local), f32),
            jax.ShapeDtypeStruct((kept, seqs, local), bf16),
        ),
        in_specs=[vmem] * 4 + [hbm] * 9,
        out_specs=(vmem,) * 4,
        scratch_shapes=[
            pltpu.VMEM((own_count, width), bf16),
            pltpu.VMEM((kept, seqs, local), bf16),
            pltpu.VMEM(conv_taps.shape, bf16),
            pltpu.VMEM((local // LANES, LANES, LANES), bf16),
            pltpu.VMEM((local // LANES, LANES, LANES), bf16),
            pltpu.VMEM((seqs, local), f32),
            dma((6,)),
            pltpu.VMEM((group, half), bf16),
            pltpu.VMEM((width, local), bf16),
            pltpu.VMEM((width, local), bf16),
            pltpu.VMEM((local, width), bf16),
            pltpu.VMEM((group, half + LANES), bf16),
            pltpu.VMEM((group // 2, half + LANES), bf16),
            pltpu.VMEM((group // 2, half + LANES), bf16),
            pltpu.VMEM((z_count, 16, half + LANES), bf16),
            dma((3,)), dma((z_count,)), dma((z_count,)), dma((tp_count,)),
            dma, dma, dma((z_count,)), dma((z_count,)),
        ],
        compiler_params=pltpu.CompilerParams(
            collective_id=0, has_side_effects=True, vmem_limit_bytes=VMEM_LIMIT
        ),
        name="mix",
    )(
        first_gain, decay_logit[None], rec_gain[None], second_gain,
        tokens, jnp.transpose(conv_state, (1, 0, 2)), conv_taps, block_decay, block_input,
        rec_state, proj_input, proj_gate, proj_out,
    )
    new_conv = jnp.transpose(conv_major, (1, 0, 2))

    shards = tp_count * ep_count
    rows = shards * 16
    side = rows // 2
    slots = local_experts * shards * 2
    wide = width // CHUNKS
    narrow = wide // 2
    result = pl.pallas_call(
        functools.partial(expert_kernel, z_count, ep_count),
        out_shape=jax.ShapeDtypeStruct((own_count, width), bf16),
        in_specs=[vmem] + [hbm] * 5,
        out_specs=vmem,
        scratch_shapes=[
            pltpu.VMEM((own_count, width), f32),
            dma((2,)),
            pltpu.VMEM((rows, half + LANES), bf16),
            pltpu.VMEM((local_experts, width, units), bf16),
            pltpu.VMEM((local_experts, width, units), bf16),
            pltpu.VMEM((local_experts, units, width), bf16),
            pltpu.VMEM((2, slots, rows), bf16),
            pltpu.VMEM((shards * 8, slots), bf16),
            pltpu.VMEM((slots, width), bf16),
            pltpu.VMEM((slots, units), bf16),
            pltpu.VMEM((slots, wide), bf16),
            pltpu.VMEM((CHUNKS, rows, narrow), bf16),
            pltpu.VMEM((CHUNKS, side, narrow), bf16),
            pltpu.VMEM((CHUNKS, side, narrow), bf16),
            pltpu.VMEM((CHUNKS, ep_count, 16 * z_count, narrow), bf16),
            pltpu.VMEM((CHUNKS, 16 * z_count, narrow), bf16),
            pltpu.VMEM((CHUNKS, z_count, 16, narrow), bf16),
            dma((local_experts,)), dma((local_experts,)), dma((local_experts,)),
            dma((z_count,)), dma((z_count, ep_count)), dma((z_count, ep_count)), dma((shards,)),
            dma((CHUNKS,)), dma((CHUNKS,)),
            dma((CHUNKS, ep_count)), dma((CHUNKS, ep_count)),
            dma((CHUNKS, z_count)), dma((CHUNKS, z_count)),
        ],
        compiler_params=pltpu.CompilerParams(
            collective_id=1, has_side_effects=True, vmem_limit_bytes=VMEM_LIMIT
        ),
        name="experts",
    )(spread_weights, second, residual, expert_gate, expert_up, expert_down)
    return (result, new_state, new_conv)


def per_device(*args):
    tokens, rec_state, ids, block = args[0], args[1], args[3], args[10]
    tp_count, ep_count = lax.axis_size("tp"), lax.axis_size("ep")
    shards = tp_count * ep_count
    expert_rows = args[15].shape[0] * shards * 2
    fits = (
        tokens.shape[0] == 8
        and tp_count % 2 == 0
        and tp_count >= 8
        and max(2, tokens.shape[0] * ids.shape[1] // EXPERTS) == 2
        and expert_rows <= 256
        and block.shape[1] == LANES
        and rec_state.shape[1] % LANES == 0
    )
    return kernel_plan(*args) if fits else collective_plan(*args)


def solution(mesh):
    in_specs = (
        P(("ep", "tp"), None),
        P("ep", "tp"),
        P("ep", None, "tp"),
        P("ep", None),
        P(("ep", "tp"), None),
        P(),
        P(None, "tp"),
        P(None, "tp"),
        P(),
        P(),
        P(),
        P(),
        P(),
        P("tp", None),
        P(),
        P("ep", None, "tp"),
        P("ep", None, "tp"),
        P("ep", "tp", None),
    )
    out_specs = (P(("ep", "tp"), None), P("ep", "tp"), P("ep", None, "tp"))
    return jax.shard_map(
        per_device, mesh=mesh, in_specs=in_specs, out_specs=out_specs, check_vma=False
    )
```
